32 devices in a mesh: grp: 2 (over y), fs: 4 (over z), tp: 4 (over x, core).
Axes of the slice: x: 2, y: 2, z: 4, core: 2. Of those that a mesh axis runs over, the one named last changes fastest.
Arguments:
- tokens: bfloat16 [4096, 2048], P(('grp', 'fs'), 'tp'), parts along dimension 0, may hold values from -36 to 36
- query_matrix: bfloat16 [2048, 1024], P('fs', 'tp'), may hold values from -0.125 to 0.125
- key_weight: bfloat16 [2048, 1024], P('fs', 'tp'), may hold values from -0.125 to 0.125
- value_weight: bfloat16 [2048, 2048], P('fs', 'tp'), may hold values from -0.125 to 0.125
- forget_lower_factor: bfloat16 [2048, 32], replicated, may hold values from -0.125 to 0.125
- decay_up: bfloat16 [32, 1024], replicated, may hold values from -1 to 1
- decay_bias: float32 [1024], replicated, may hold values from -1 to 8
- log_extra: float32 [4096, 1024], P(('grp', 'fs'), 'tp'), parts along dimension 0, may hold values from -0.7 to 0
- head_gain: float32 [256], replicated, may hold values from 0.1 to 1.9
- out_weight: bfloat16 [2048, 2048], P('tp', 'fs'), may hold values from -0.125 to 0.125
- mix_gain: float32 [2048], P('tp'), may hold values from 0.1 to 1.9
- up_weight: bfloat16 [2048, 8192], P('fs', 'tp'), may hold values from -0.125 to 0.125
- down_weight: bfloat16 [8192, 2048], P('tp', 'fs'), may hold values from -0.0625 to 0.0625
- out_gain: float32 [2048], P('tp'), may hold values from 0.1 to 1.9
Outputs:
- layer_out: bfloat16 [4096, 2048], P(('grp', 'fs'), 'tp'), parts along dimension 0
The draws below stay inside these ranges and needn't reach their ends.
There are 2 independent parts, one for each index of `grp`. The reference program is written for one: setup_inputs(seed, part) draws one part's arguments, and reference() takes and returns one part's arrays. A program takes and returns all parts, laid end to end along the dimension named above; an argument that names none is the same for every part. Nothing has to cross between parts.
All inputs are finite; a program needn't handle non-finite values.
Results may differ from the reference program's by a relative error of at most 0.015.
Values may be sent and summed in bfloat16 or wider, within the bound.
A program may use at most 64 MiB of HBM per device.

```python
import math
import jax
import jax.numpy as jnp
from jax import lax

D = 2048
HEADS = 8
DK = 128
DV = 256
FF = 8192
RANK = 32
SEGMENT_LENGTH = 64
SEQ = 512
OVERALL_WORDS = 2048
N_TP = 4


def draw_tokens(key, part):
    address_embeddings = jax.random.split(key, 3)
    column_index = jnp.arange(D).astype(jnp.float32)
    col_scale = 3.0 ** (column_index / (D - 1)) * jnp.exp(jax.random.uniform(address_embeddings[1], (D,), jnp.float32, 0.0, math.log(1.5))) / 1.5
    row_scale = jnp.exp(jax.random.uniform(address_embeddings[2], (OVERALL_WORDS, 1), jnp.float32, 0.0, math.log(2.0)))
    base = jnp.clip(jax.random.normal(address_embeddings[0], (OVERALL_WORDS, D), jnp.float32), -6.0, 6.0)
    return (base * col_scale * row_scale).astype(jnp.bfloat16)


def draw_decay_bias(key, part):
    address_embeddings = jax.random.split(key, 3)
    width = HEADS * DK
    picked = jax.random.randint(address_embeddings[0], (width,), 0, 2)
    fast = jax.random.uniform(address_embeddings[1], (width,), jnp.float32, -1.0, 1.5)
    slow = jax.random.uniform(address_embeddings[2], (width,), jnp.float32, 4.0, 7.0)
    return jnp.where(picked == 1, fast, slow)


def draw_log_extra(key, part):
    address_embeddings = jax.random.split(key, 3)
    width = HEADS * DK
    forget_speeds = jnp.exp(jax.random.uniform(address_embeddings[0], (OVERALL_WORDS // SEGMENT_LENGTH, width), jnp.float32, math.log(0.0005), math.log(0.004)))
    word_segments = jax.random.randint(address_embeddings[1], (OVERALL_WORDS, 1), 0, 128) == 0
    forget_intensity = jax.random.uniform(address_embeddings[2], (OVERALL_WORDS, width), jnp.float32, math.log(0.5), math.log(0.8))
    return -jnp.repeat(forget_speeds, SEGMENT_LENGTH, axis=0) + jnp.where(word_segments, forget_intensity, 0.0)


def block_levels(stream_key, dims, cuts, low, high):
    level, own = 1.0, jax.random.fold_in(stream_key, 6)
    for axis_at, shards_of in cuts:
        heights = jnp.exp(jax.random.uniform(jax.random.fold_in(own, axis_at), (shards_of,), jnp.float32, low / len(cuts), high / len(cuts)))
        level = level * jnp.repeat(heights, dims[axis_at] // shards_of).reshape([-1 if axis == axis_at else 1 for axis in range(len(dims))])
    return level


def noise(stream_key, shape, scale, bound, cuts=(), dtype=jnp.bfloat16):
    values = scale * jax.random.normal(stream_key, shape, jnp.float32)
    if cuts:
        values = values * block_levels(stream_key, shape, cuts, -0.22, 0.18)
    return jnp.clip(values, -bound, bound).astype(dtype)


def setup_inputs(seed: int = 0, part: int = 0) -> dict:
    keys = jax.random.split(jax.random.key(seed), 15)
    part_keys = jax.random.split(jax.random.fold_in(keys[14], part), 15)
    tokens = draw_tokens(jax.random.fold_in(jax.random.fold_in(keys[14], part), 71), part)
    query_matrix = noise(keys[1], (D, HEADS * DK), D ** -0.5, 0.125, ((0, 4), (1, 4)))
    key_weight = noise(keys[2], (D, HEADS * DK), D ** -0.5, 0.125, ((0, 4), (1, 4)))
    value_weight = noise(keys[3], (D, HEADS * DV), D ** -0.5, 0.125, ((0, 4), (1, 4)))
    forget_lower_factor = noise(keys[4], (D, RANK), D ** -0.5, 0.125)
    decay_up = noise(keys[5], (RANK, HEADS * DK), RANK ** -0.5, 1.0)
    decay_bias = draw_decay_bias(jax.random.fold_in(keys[14], 71), part)
    log_extra = draw_log_extra(jax.random.fold_in(jax.random.fold_in(keys[14], part), 71), part)
    head_gain = jnp.clip(1.0 + 0.18 * jax.random.normal(keys[8], (DV,), jnp.float32), 0.1, 1.9)
    out_weight = noise(keys[9], (HEADS * DV, D), (HEADS * DV) ** -0.5, 0.125, ((0, 4), (1, 4)))
    mix_gain = jnp.clip(1.0 + 0.18 * jax.random.normal(keys[10], (D,), jnp.float32), 0.1, 1.9)
    up_weight = noise(keys[11], (D, FF), D ** -0.5, 0.125, ((0, 4), (1, 4)))
    down_weight = noise(keys[12], (FF, D), FF ** -0.5, 0.0625, ((0, 4), (1, 4)))
    out_gain = jnp.clip(1.0 + 0.18 * jax.random.normal(keys[13], (D,), jnp.float32), 0.1, 1.9)
    return {"tokens": tokens, "query_matrix": query_matrix, "key_weight": key_weight, "value_weight": value_weight, "forget_lower_factor": forget_lower_factor, "decay_up": decay_up, "decay_bias": decay_bias, "log_extra": log_extra, "head_gain": head_gain, "out_weight": out_weight, "mix_gain": mix_gain, "up_weight": up_weight, "down_weight": down_weight, "out_gain": out_gain}


ALPHA = 2.0 ** 0.5
TAU = 16.0
EPS = 1e-05
HIGH = lax.Precision.HIGHEST

def block_scan(queries, key_rows, value_rows, log_decay):
    span = queries.shape[2]
    causal = (jnp.arange(span)[:, None] >= jnp.arange(span)[None, :])[:, :, None]

    def step(state, inputs):
        query_block, key_block, value_block, decay_block = inputs
        cumul = jnp.cumsum(decay_block, axis=1)
        last_cum = cumul[:, -1:, :]
        carried = jnp.einsum('hcd,hde->hce', query_block * jnp.exp(cumul), state, precision=HIGH)
        differ = cumul[:, :, None, :] - cumul[:, None, :, :]
        weights = jnp.exp(jnp.where(causal, differ, -jnp.inf))
        scores = lax.optimization_barrier(jnp.sum(query_block[:, :, None, :] * key_block[:, None, :, :] * weights, axis=-1))
        within = jnp.einsum('hij,hje->hie', scores, value_block, precision=HIGH)
        fresh = jnp.einsum('hcd,hce->hde', key_block * jnp.exp(last_cum - cumul), value_block, precision=HIGH)
        new_state = jnp.exp(last_cum[:, 0, :])[:, :, None] * state + fresh
        return (new_state, carried + within)
    start = jnp.zeros((queries.shape[1], queries.shape[3], value_rows.shape[3]), jnp.float32)
    _, outputs = lax.scan(step, start, (queries, key_rows, value_rows, log_decay))
    return outputs

def mixer_sequence(inputs):
    queries, key_rows, value_rows, log_decay = inputs
    count = queries.shape[0] // SEGMENT_LENGTH

    def blocks(array, depth):
        return array.astype(jnp.float32).reshape(count, SEGMENT_LENGTH, HEADS, depth).transpose(0, 2, 1, 3)
    outputs = block_scan(blocks(queries, DK) * DK ** (-0.5), blocks(key_rows, DK), blocks(value_rows, DV), blocks(log_decay, DK))
    return outputs.transpose(0, 2, 1, 3).reshape(queries.shape[0], HEADS, DV)

def group_sum(left, right, width):
    running = jnp.zeros((left.shape[0], right.shape[1]), jnp.float32)
    for index in range(N_TP):
        partial_sum = jnp.dot(left[:, index * width:(index + 1) * width], right[index * width:(index + 1) * width], preferred_element_type=jnp.float32).astype(jnp.bfloat16)
        partial_sum = lax.optimization_barrier(partial_sum)
        running = running + partial_sum.astype(jnp.float32)
    return running

def layer_norm(summed, gain_cols):
    row_mean = lax.optimization_barrier(jnp.mean(summed, axis=1, keepdims=True))
    centered = summed - row_mean
    row_var = lax.optimization_barrier(jnp.mean(centered * centered, axis=1, keepdims=True))
    return (centered * lax.rsqrt(row_var + EPS) * gain_cols).astype(jnp.bfloat16)

def reference(tokens, query_matrix, key_weight, value_weight, forget_lower_factor, decay_up, decay_bias, log_extra, head_gain, out_weight, mix_gain, up_weight, down_weight, out_gain):
    queries = jnp.dot(tokens, query_matrix, preferred_element_type=jnp.float32).astype(jnp.bfloat16)
    key_rows = jnp.dot(tokens, key_weight, preferred_element_type=jnp.float32).astype(jnp.bfloat16)
    value_rows = jnp.dot(tokens, value_weight, preferred_element_type=jnp.float32).astype(jnp.bfloat16)
    low = jnp.dot(tokens, forget_lower_factor, preferred_element_type=jnp.float32).astype(jnp.bfloat16)
    gate_pre = jnp.dot(low, decay_up, preferred_element_type=jnp.float32) + decay_bias
    log_decay = jax.nn.log_sigmoid(gate_pre) / TAU + log_extra
    count = tokens.shape[0] // SEQ
    attended = lax.map(mixer_sequence, (queries.reshape(count, SEQ, HEADS * DK), key_rows.reshape(count, SEQ, HEADS * DK), value_rows.reshape(count, SEQ, HEADS * DV), log_decay.reshape(count, SEQ, HEADS * DK)))
    attended = attended.reshape(tokens.shape[0], HEADS, DV)
    scaled = attended * lax.rsqrt(lax.optimization_barrier(jnp.mean(attended * attended, axis=-1, keepdims=True)) + EPS) * head_gain
    mixed_heads = scaled.reshape(tokens.shape[0], HEADS * DV).astype(jnp.bfloat16)
    mix = group_sum(mixed_heads, out_weight, HEADS * DV // N_TP)
    normed = layer_norm(ALPHA * tokens.astype(jnp.float32) + mix, mix_gain)
    hidden = jnp.dot(normed, up_weight, preferred_element_type=jnp.float32)
    activation = jnp.square(jax.nn.relu(hidden)).astype(jnp.bfloat16)
    down = group_sum(activation, down_weight, FF // N_TP)
    return layer_norm(ALPHA * normed.astype(jnp.float32) + down, out_gain)
```

```python
import functools

import jax
import jax.numpy as jnp
from jax import lax
from jax.experimental import pallas as pl
from jax.experimental.pallas import tpu as pltpu
from jax.sharding import PartitionSpec as P

DK = 128
DV = 256
CHUNK = 64
SUB = 16

ALPHA = 2.0**0.5
TAU = 16.0
EPS = 1e-05


def shift(array, axis, size, step):
    return lax.ppermute(array, axis, [(i, (i + step) % size) for i in range(size)])


def gather_shards(weight, n, groups):
    rows, cols = weight.shape
    paired = groups % 2 == 0
    parts = 2 if paired else 1
    halves = weight.reshape(parts, rows // parts, cols)
    me = lax.axis_index("fs")
    side = lax.rem(lax.axis_index("grp"), 2) if paired else 0
    mine = lax.dynamic_index_in_dim(halves, side, 0, keepdims=False) if paired else weight
    full = jnp.zeros((n, parts, rows // parts, cols), weight.dtype)
    full = lax.dynamic_update_slice(full, halves[None], (me, 0, 0, 0))
    height = rows // parts

    def place(full, piece, owner, at):
        full = lax.dynamic_update_slice(full, piece[None, None], (owner, side, at, 0))
        if paired:
            swapped = lax.ppermute(piece, "grp", [(g, g ^ 1) for g in range(groups)])
            full = lax.dynamic_update_slice(full, swapped[None, None], (owner, 1 - side, at, 0))
        return full

    right, left = mine, mine
    for distance in range(1, n // 2 + 1):
        at_right, at_left = 0, 0
        if 2 * distance == n:
            right, left, at_left = right[: height // 2], left[height // 2 :], height // 2
        right = shift(right, "fs", n, 1)
        full = place(full, right, lax.rem(me - distance + n, n), at_right)
        left = shift(left, "fs", n, -1)
        full = place(full, left, lax.rem(me + distance, n), at_left)
    return full.reshape(n, rows, cols)


def scan_kernel(heads, qkv_ref, low_ref, up_ref, bias_ref, extra_ref, gain_ref, out_ref, decay_ref):
    rows = qkv_ref.shape[0]
    gate = jnp.dot(low_ref[...], up_ref[...], preferred_element_type=jnp.float32) + bias_ref[...]
    logsig = jnp.minimum(gate, 0.0) - jnp.log1p(jnp.exp(-jnp.abs(gate)))
    decay_ref[...] = logsig / TAU + extra_ref[...]
    at_row = lax.broadcasted_iota(jnp.int32, (CHUNK, CHUNK), 0)
    at_col = lax.broadcasted_iota(jnp.int32, (CHUNK, CHUNK), 1)
    tri = (at_row >= at_col).astype(jnp.float32)
    sub_row = lax.broadcasted_iota(jnp.int32, (SUB, SUB), 0)
    sub_col = lax.broadcasted_iota(jnp.int32, (SUB, SUB), 1)
    gain = gain_ref[...]
    nt = (((1,), (1,)), ((), ()))
    tn = (((0,), (0,)), ((), ()))

    def step(index, states):
        at = pl.multiple_of(index * CHUNK, CHUNK)
        here = pl.ds(at, CHUNK)
        fresh_states = []
        for head in range(heads):
            query = qkv_ref[here, head * DK : (head + 1) * DK].astype(jnp.float32) * DK**-0.5
            keys = qkv_ref[here, (heads + head) * DK : (heads + head + 1) * DK].astype(jnp.float32)
            at_value = 2 * heads * DK + head * DV
            value = qkv_ref[here, at_value : at_value + DV]
            decay = decay_ref[here, head * DK : (head + 1) * DK]
            cumul = jnp.dot(
                tri, decay, precision=lax.Precision.HIGHEST, preferred_element_type=jnp.float32
            )
            last = cumul[CHUNK - 1 : CHUNK, :]
            state = states[head]
            out = lax.dot_general(
                (query * jnp.exp(cumul)).astype(jnp.bfloat16),
                state.astype(jnp.bfloat16),
                nt,
                preferred_element_type=jnp.float32,
            )
            strips = []
            for a in range(CHUNK // SUB):
                lo, hi = a * SUB, (a + 1) * SUB
                q_a, k_a, g_a = query[lo:hi], keys[lo:hi], cumul[lo:hi]
                diag = jnp.zeros((SUB, SUB), jnp.float32)
                for j in range(SUB):
                    weight = jnp.exp(jnp.minimum(g_a - g_a[j : j + 1], 0.0))
                    column = jnp.sum(q_a * k_a[j : j + 1] * weight, axis=1, keepdims=True)
                    diag = jnp.where((sub_col == j) & (sub_row >= j), column, diag)
                pieces = [diag.astype(jnp.bfloat16)]
                if a:
                    base = cumul[lo - 1 : lo]
                    before = lax.dot_general(
                        (q_a * jnp.exp(g_a - base)).astype(jnp.bfloat16),
                        (keys[:lo] * jnp.exp(base - cumul[:lo])).astype(jnp.bfloat16),
                        nt,
                        preferred_element_type=jnp.float32,
                    )
                    pieces.insert(0, before.astype(jnp.bfloat16))
                strip = jnp.dot(
                    pieces[-1], value[lo:hi], preferred_element_type=jnp.float32
                )
                if a:
                    strip += jnp.dot(pieces[0], value[:lo], preferred_element_type=jnp.float32)
                strips.append(strip)
            out = out + jnp.concatenate(strips, axis=0)
            fresh = lax.dot_general(
                value,
                (keys * jnp.exp(last - cumul)).astype(jnp.bfloat16),
                tn,
                preferred_element_type=jnp.float32,
            )
            fresh_states.append(state * jnp.exp(last) + fresh)
            mean = jnp.mean(out * out, axis=1, keepdims=True)
            out_ref[here, head * DV : (head + 1) * DV] = (
                out * lax.rsqrt(mean + EPS) * gain
            ).astype(jnp.bfloat16)
        return tuple(fresh_states)

    start = tuple(jnp.zeros((DV, DK), jnp.float32) for _ in range(heads))
    lax.fori_loop(0, rows // CHUNK, step, start)


def scan_heads(qkv, low, local_up, local_bias, extra, gain, heads):
    rows = qkv.shape[0]
    vmem = pl.BlockSpec(memory_space=pltpu.VMEM)
    return pl.pallas_call(
        functools.partial(scan_kernel, heads),
        out_shape=jax.ShapeDtypeStruct((rows, heads * DV), jnp.bfloat16),
        in_specs=[vmem] * 6,
        out_specs=vmem,
        scratch_shapes=[pltpu.VMEM((rows, heads * DK), jnp.float32)],
        cost_estimate=pl.CostEstimate(
            flops=20_000_000_000, bytes_accessed=4_000_000, transcendentals=0
        ),
        name="scan",
    )(qkv, low, local_up, local_bias, extra, gain)


def layer_norm(summed, gain_cols):
    row_total, row_squares = lax.psum(
        (jnp.sum(summed, axis=1), jnp.sum(summed * summed, axis=1)), "tp"
    )
    width = summed.shape[1] * lax.psum(1, "tp")
    row_mean = row_total / width
    row_var = row_squares / width - row_mean * row_mean
    centered = summed - row_mean[:, None]
    return (centered * lax.rsqrt(row_var[:, None] + EPS) * gain_cols).astype(jnp.bfloat16)


def column_dots(rows, shards):
    return jnp.concatenate(
        [
            jnp.dot(rows, shards[p], preferred_element_type=jnp.float32).astype(jnp.bfloat16)
            for p in range(shards.shape[0])
        ],
        axis=1,
    )


def local(
    n_fs,
    n_grp,
    tokens,
    query_matrix,
    key_weight,
    value_weight,
    forget_lower_factor,
    decay_up,
    decay_bias,
    log_extra,
    head_gain,
    out_weight,
    mix_gain,
    up_weight,
    down_weight,
    out_gain,
):
    gather = functools.partial(gather_shards, n=n_fs, groups=n_grp)
    key_cols = query_matrix.shape[1]
    local_heads = key_cols // DK
    gathered = lax.all_gather(tokens, "tp", axis=1, tiled=True)
    qkv_shards = gather(jnp.concatenate([query_matrix, key_weight, value_weight], axis=1))
    out_shards = gather(out_weight)
    up_shards = gather(up_weight)
    down_shards = gather(down_weight)

    qkv_full = qkv_shards.reshape(-1, qkv_shards.shape[2])
    qkv = jnp.dot(gathered, qkv_full, preferred_element_type=jnp.float32).astype(jnp.bfloat16)
    low = jnp.dot(gathered, forget_lower_factor, preferred_element_type=jnp.float32).astype(
        jnp.bfloat16
    )
    offset_cols = lax.axis_index("tp") * key_cols
    local_up = lax.dynamic_slice_in_dim(decay_up, offset_cols, key_cols, 1)
    local_bias = lax.dynamic_slice_in_dim(decay_bias, offset_cols, key_cols, 0)
    mixed_heads = scan_heads(
        qkv, low, local_up, local_bias[None], log_extra, head_gain[None], local_heads
    )
    mix = lax.psum_scatter(
        column_dots(mixed_heads, out_shards), "tp", scatter_dimension=1, tiled=True
    ).astype(jnp.float32)
    normed_local = layer_norm(ALPHA * tokens.astype(jnp.float32) + mix, mix_gain)
    normed_rows = lax.all_gather(normed_local, "tp", axis=1, tiled=True)
    up_full = up_shards.reshape(-1, up_shards.shape[2])
    hidden = jnp.dot(normed_rows, up_full, preferred_element_type=jnp.float32)
    activation = jnp.square(jax.nn.relu(hidden)).astype(jnp.bfloat16)
    down = lax.psum_scatter(
        column_dots(activation, down_shards), "tp", scatter_dimension=1, tiled=True
    ).astype(jnp.float32)
    return layer_norm(ALPHA * normed_local.astype(jnp.float32) + down, out_gain)


def solution(mesh):
    in_specs = (
        P(("grp", "fs"), "tp"),
        P("fs", "tp"),
        P("fs", "tp"),
        P("fs", "tp"),
        P(),
        P(),
        P(),
        P(("grp", "fs"), "tp"),
        P(),
        P("tp", "fs"),
        P("tp"),
        P("fs", "tp"),
        P("tp", "fs"),
        P("tp"),
    )
    out_specs = P(("grp", "fs"), "tp")
    body = functools.partial(local, mesh.shape["fs"], mesh.shape["grp"])
    return jax.shard_map(body, mesh=mesh, in_specs=in_specs, out_specs=out_specs, check_vma=False)
```

```python
import functools

import jax
import jax.numpy as jnp
from jax import lax
from jax.experimental import pallas as pl
from jax.experimental.pallas import tpu as pltpu
from jax.sharding import PartitionSpec as P

DK = 128
DV = 256
CHUNK = 64
SUB = 16

ALPHA = 2.0**0.5
TAU = 16.0
EPS = 1e-05


def shift(array, axis, size, step):
    return lax.ppermute(array, axis, [(i, (i + step) % size) for i in range(size)])


class Gather:
    def __init__(self, weight, n, groups):
        rows, cols = weight.shape
        self.n, self.groups, self.shape = n, groups, (n, rows, cols)
        self.paired = groups % 2 == 0
        parts = 2 if self.paired else 1
        self.height = rows // parts
        halves = weight.reshape(parts, self.height, cols)
        self.me = lax.axis_index("fs")
        self.side = lax.rem(lax.axis_index("grp"), 2) if self.paired else 0
        mine = weight
        if self.paired:
            mine = lax.dynamic_index_in_dim(halves, self.side, 0, keepdims=False)
        self.right, self.left = mine, mine
        full = jnp.zeros((n, parts, self.height, cols), weight.dtype)
        self.full = lax.dynamic_update_slice(full, halves[None], (self.me, 0, 0, 0))

    def place(self, piece, owner, at):
        self.full = lax.dynamic_update_slice(
            self.full, piece[None, None], (owner, self.side, at, 0)
        )
        if self.paired:
            swapped = lax.ppermute(piece, "grp", [(g, g ^ 1) for g in range(self.groups)])
            self.full = lax.dynamic_update_slice(
                self.full, swapped[None, None], (owner, 1 - self.side, at, 0)
            )

    def hop(self, distance, after):
        n, me, height = self.n, self.me, self.height
        right, left = self.right, self.left
        at_left = 0
        if 2 * distance == n:
            right, left, at_left = right[: height // 2], left[height // 2 :], height // 2
        if after is not None:
            right, left, _, _ = lax.optimization_barrier((right, left) + after)
        self.right, self.left = shift(right, "fs", n, 1), shift(left, "fs", n, -1)
        self.place(self.right, lax.rem(me - distance + n, n), 0)
        self.place(self.left, lax.rem(me + distance, n), at_left)
        return self.right, self.left

    def result(self):
        return self.full.reshape(self.shape)


def gather_all(chunks, n, groups):
    rings = [Gather(chunk, n, groups) for chunk in chunks]
    hops = n // 2
    order = sorted(
        (c * hops / 2 + (d - 1) * 1.5, c, d)
        for c in range(len(rings))
        for d in range(1, hops + 1)
    )
    sent = []
    for _, c, d in order:
        sent.append(rings[c].hop(d, sent[-2] if len(sent) > 1 else None))
    return [ring.result() for ring in rings]


def scan_kernel(heads, qkv_ref, low_ref, up_ref, bias_ref, extra_ref, gain_ref, out_ref, decay_ref):
    rows = qkv_ref.shape[0]
    gate = jnp.dot(low_ref[...], up_ref[...], preferred_element_type=jnp.float32) + bias_ref[...]
    logsig = jnp.minimum(gate, 0.0) - jnp.log1p(jnp.exp(-jnp.abs(gate)))
    decay_ref[...] = logsig / TAU + extra_ref[...]
    at_row = lax.broadcasted_iota(jnp.int32, (CHUNK, CHUNK), 0)
    at_col = lax.broadcasted_iota(jnp.int32, (CHUNK, CHUNK), 1)
    tri = (at_row >= at_col).astype(jnp.float32)
    sub_row = lax.broadcasted_iota(jnp.int32, (SUB, SUB), 0)
    sub_col = lax.broadcasted_iota(jnp.int32, (SUB, SUB), 1)
    gain = gain_ref[...]
    nt = (((1,), (1,)), ((), ()))
    tn = (((0,), (0,)), ((), ()))

    def step(index, states):
        at = pl.multiple_of(index * CHUNK, CHUNK)
        here = pl.ds(at, CHUNK)
        fresh_states = []
        for head in range(heads):
            query = qkv_ref[here, head * DK : (head + 1) * DK].astype(jnp.float32) * DK**-0.5
            keys = qkv_ref[here, (heads + head) * DK : (heads + head + 1) * DK].astype(jnp.float32)
            at_value = 2 * heads * DK + head * DV
            value = qkv_ref[here, at_value : at_value + DV]
            decay = decay_ref[here, head * DK : (head + 1) * DK]
            cumul = jnp.dot(
                tri, decay, precision=lax.Precision.HIGHEST, preferred_element_type=jnp.float32
            )
            last = cumul[CHUNK - 1 : CHUNK, :]
            state = states[head]
            out = lax.dot_general(
                (query * jnp.exp(cumul)).astype(jnp.bfloat16),
                state.astype(jnp.bfloat16),
                nt,
                preferred_element_type=jnp.float32,
            )
            strips = []
            for a in range(CHUNK // SUB):
                lo, hi = a * SUB, (a + 1) * SUB
                q_a, k_a, g_a = query[lo:hi], keys[lo:hi], cumul[lo:hi]
                diag = jnp.zeros((SUB, SUB), jnp.float32)
                for j in range(SUB):
                    weight = jnp.exp(jnp.minimum(g_a - g_a[j : j + 1], 0.0))
                    column = jnp.sum(q_a * k_a[j : j + 1] * weight, axis=1, keepdims=True)
                    diag = jnp.where((sub_col == j) & (sub_row >= j), column, diag)
                pieces = [diag.astype(jnp.bfloat16)]
                if a:
                    base = cumul[lo - 1 : lo]
                    before = lax.dot_general(
                        (q_a * jnp.exp(g_a - base)).astype(jnp.bfloat16),
                        (keys[:lo] * jnp.exp(base - cumul[:lo])).astype(jnp.bfloat16),
                        nt,
                        preferred_element_type=jnp.float32,
                    )
                    pieces.insert(0, before.astype(jnp.bfloat16))
                strip = jnp.dot(
                    pieces[-1], value[lo:hi], preferred_element_type=jnp.float32
                )
                if a:
                    strip += jnp.dot(pieces[0], value[:lo], preferred_element_type=jnp.float32)
                strips.append(strip)
            out = out + jnp.concatenate(strips, axis=0)
            fresh = lax.dot_general(
                value,
                (keys * jnp.exp(last - cumul)).astype(jnp.bfloat16),
                tn,
                preferred_element_type=jnp.float32,
            )
            fresh_states.append(state * jnp.exp(last) + fresh)
            mean = jnp.mean(out * out, axis=1, keepdims=True)
            out_ref[here, head * DV : (head + 1) * DV] = (
                out * lax.rsqrt(mean + EPS) * gain
            ).astype(jnp.bfloat16)
        return tuple(fresh_states)

    start = tuple(jnp.zeros((DV, DK), jnp.float32) for _ in range(heads))
    lax.fori_loop(0, rows // CHUNK, step, start)


def scan_heads(qkv, low, local_up, local_bias, extra, gain, heads):
    rows = qkv.shape[0]
    vmem = pl.BlockSpec(memory_space=pltpu.VMEM)
    return pl.pallas_call(
        functools.partial(scan_kernel, heads),
        out_shape=jax.ShapeDtypeStruct((rows, heads * DV), jnp.bfloat16),
        in_specs=[vmem] * 6,
        out_specs=vmem,
        scratch_shapes=[pltpu.VMEM((rows, heads * DK), jnp.float32)],
        cost_estimate=pl.CostEstimate(
            flops=20_000_000_000, bytes_accessed=4_000_000, transcendentals=0
        ),
        name="scan",
    )(qkv, low, local_up, local_bias, extra, gain)


def layer_norm(summed, gain_cols):
    row_total, row_squares = lax.psum(
        (jnp.sum(summed, axis=1), jnp.sum(summed * summed, axis=1)), "tp"
    )
    width = summed.shape[1] * lax.psum(1, "tp")
    row_mean = row_total / width
    row_var = row_squares / width - row_mean * row_mean
    centered = summed - row_mean[:, None]
    return (centered * lax.rsqrt(row_var[:, None] + EPS) * gain_cols).astype(jnp.bfloat16)


def column_dots(rows, chunks):
    return jnp.concatenate(
        [
            jnp.dot(rows, shards[p], preferred_element_type=jnp.float32).astype(jnp.bfloat16)
            for p in range(chunks[0].shape[0])
            for shards in chunks
        ],
        axis=1,
    )


def local(
    n_fs,
    n_grp,
    tokens,
    query_matrix,
    key_weight,
    value_weight,
    forget_lower_factor,
    decay_up,
    decay_bias,
    log_extra,
    head_gain,
    out_weight,
    mix_gain,
    up_weight,
    down_weight,
    out_gain,
):
    key_cols = query_matrix.shape[1]
    local_heads = key_cols // DK
    gathered = lax.all_gather(tokens, "tp", axis=1, tiled=True)
    qkv_weight = jnp.concatenate([query_matrix, key_weight, value_weight], axis=1)
    half_up, half_down = up_weight.shape[1] // 2, down_weight.shape[1] // 2
    qkv_shards, out_shards, up_a, up_b, down_a, down_b = gather_all(
        [
            qkv_weight,
            out_weight,
            up_weight[:, :half_up],
            up_weight[:, half_up:],
            down_weight[:, :half_down],
            down_weight[:, half_down:],
        ],
        n_fs,
        n_grp,
    )

    qkv_full = qkv_shards.reshape(-1, qkv_shards.shape[2])
    qkv = jnp.dot(gathered, qkv_full, preferred_element_type=jnp.float32).astype(jnp.bfloat16)
    low = jnp.dot(gathered, forget_lower_factor, preferred_element_type=jnp.float32).astype(
        jnp.bfloat16
    )
    offset_cols = lax.axis_index("tp") * key_cols
    local_up = lax.dynamic_slice_in_dim(decay_up, offset_cols, key_cols, 1)
    local_bias = lax.dynamic_slice_in_dim(decay_bias, offset_cols, key_cols, 0)
    mixed_heads = scan_heads(
        qkv, low, local_up, local_bias[None], log_extra, head_gain[None], local_heads
    )
    mix = lax.psum_scatter(
        column_dots(mixed_heads, [out_shards]), "tp", scatter_dimension=1, tiled=True
    ).astype(jnp.float32)
    normed_local = layer_norm(ALPHA * tokens.astype(jnp.float32) + mix, mix_gain)
    normed_rows = lax.all_gather(normed_local, "tp", axis=1, tiled=True)
    activation = jnp.concatenate(
        [
            jnp.square(
                jax.nn.relu(
                    jnp.dot(
                        normed_rows,
                        shards.reshape(-1, half_up),
                        preferred_element_type=jnp.float32,
                    )
                )
            ).astype(jnp.bfloat16)
            for shards in (up_a, up_b)
        ],
        axis=1,
    )
    down = lax.psum_scatter(
        column_dots(activation, [down_a, down_b]), "tp", scatter_dimension=1, tiled=True
    ).astype(jnp.float32)
    return layer_norm(ALPHA * normed_local.astype(jnp.float32) + down, out_gain)


def solution(mesh):
    in_specs = (
        P(("grp", "fs"), "tp"),
        P("fs", "tp"),
        P("fs", "tp"),
        P("fs", "tp"),
        P(),
        P(),
        P(),
        P(("grp", "fs"), "tp"),
        P(),
        P("tp", "fs"),
        P("tp"),
        P("fs", "tp"),
        P("tp", "fs"),
        P("tp"),
    )
    out_specs = P(("grp", "fs"), "tp")
    body = functools.partial(local, mesh.shape["fs"], mesh.shape["grp"])
    return jax.shard_map(body, mesh=mesh, in_specs=in_specs, out_specs=out_specs, check_vma=False)
```
